768 devices in a mesh: ep: 24 (over z, core), tp: 32 (over y, x).
Axes of the slice: x: 4, y: 8, z: 12, core: 2. Of those that a mesh axis runs over, the one named last changes fastest.
Arguments:
- tokens: bfloat16 [3072, 2048], P('ep'), may hold values from -6 to 6
- norm_gain: float32 [2048], replicated, may hold values from 0.1 to 1.9
- route_ids: int32 [3072, 2], P('ep'), may hold values from 0 to 23, all different within a row; in each aligned block of 128 rows (0 to 127, 128 to 255, ...) at most 16 rows name the same one
- route_weights: float32 [3072, 2], P('ep'), may hold values from 0.05 to 1
- gate_proj: bfloat16 [24, 2048, 12288], P('ep', None, 'tp'), may hold values from -0.125 to 0.125
- up_proj: bfloat16 [24, 2048, 12288], P('ep', None, 'tp'), may hold values from -0.125 to 0.125
- down_proj: bfloat16 [24, 12288, 2048], P('ep', 'tp'), may hold values from -0.0546875 to 0.0546875
Outputs:
- mixed: bfloat16 [3072, 2048], P('ep', 'tp')
The draws below stay inside these ranges and needn't reach their ends.
Inputs may be any that keep to these rules, and one draw needn't show every extreme that they name: `route_ids`: each token names 2 different experts; within the rows of one device (aligned blocks of 128 tokens) no expert is named by more than 16 pairs, a bound that some block reaches.
All inputs are finite; a program needn't handle non-finite values.
Results may differ from the reference program's by a relative error of at most 0.017.
Values may be sent and summed in bfloat16 or wider, within the bound.
A program may use at most 32 MiB of HBM per device.

```python
import math
import jax
import jax.numpy as jnp
import numpy as np
from jax import lax

D = 2048
FF = 12288
TOPK = 2
TOK_DEV = 128
EXPERTS = 24
TOKENS = 3072
CAP = 16
HID_BLOCK = 384
N_EP = 24
N_TP = 32


def levels(key, shape, cuts, smallest, largest):
    level, own = 1.0, jax.random.fold_in(key, 6)
    for axis_at, shards_of in cuts:
        draws = jnp.exp(jax.random.uniform(jax.random.fold_in(own, axis_at), (shards_of,), jnp.float32, smallest / len(cuts), largest / len(cuts)))
        level = level * jnp.repeat(draws, shape[axis_at] // shards_of).reshape([-1 if axis == axis_at else 1 for axis in range(len(shape))])
    return level


def assign_block(rng, own, number, rows, count, top, most, skew):
    ranking = jax.random.permutation(rng, count)
    packed, common = shares(count, rows * top, most, skew, True), shares(count, rows * top, most, skew, False)
    places = jnp.arange(count)

    def named(tallies, offset_by):
        used = int((tallies > 0).sum())
        fixed = max(1, used // 4)
        shifted = fixed + (places - fixed + offset_by * (used - fixed)) % max(1, count - fixed)
        return jnp.zeros((count,), jnp.int32).at[ranking[jnp.where(places < fixed, places, shifted)]].set(jnp.asarray(tallies, jnp.int32))

    tallies = jnp.where(number % 4 == 0, named(packed, number // 4), named(common, number - number // 4 - 1))
    mixed = jax.random.permutation(jax.random.fold_in(own, 3), count)
    giver, receiver = mixed[0:count // 2 * 2:2], mixed[1:count // 2 * 2:2]
    slack = jnp.minimum(tallies[giver] - 1, most - tallies[receiver]) // 2
    slack = jnp.where((giver == ranking[0]) | (receiver == ranking[0]) | (tallies[receiver] == 0), 0, jnp.maximum(slack, 0))
    shifted = jax.random.randint(jax.random.fold_in(own, 4), (count // 2,), 0, 1 << 20) % (slack + 1)
    tallies = tallies.at[giver].add(-shifted).at[receiver].add(shifted)
    members = jnp.searchsorted(jnp.cumsum(tallies), jnp.arange(rows * top), side="right").astype(jnp.int32)
    listing = members.reshape(top, rows).T
    listing = listing[jax.random.permutation(jax.random.fold_in(own, 1), rows)]
    offset_by = jax.random.randint(jax.random.fold_in(own, 2), (rows, 1), 0, top)
    return jnp.take_along_axis(listing, (jnp.arange(top)[None, :] + offset_by) % top, axis=1)


def shares(amount, total, limit, slope, full):
    portions = [(1 << 20) // math.isqrt(standing ** slope) + 1 for standing in range(1, amount + 1)]
    largest = limit if full else min(limit, max(-(-total // amount), total * portions[0] // sum(portions)))
    least = 1 if total - largest >= amount - 1 else 0
    holding, rest = [largest] + [least] * (amount - 1), total - largest - least * (amount - 1)
    while rest > 0:
        candidates = [i for i in range(1, amount) if holding[i] < largest] or [i for i in range(1, amount) if holding[i] < limit]
        whole, remaining = sum([portions[i] for i in candidates]), rest
        for i in candidates:
            addition = min(limit - holding[i], max(1, remaining * portions[i] // whole), rest)
            holding[i] = holding[i] + addition
            rest = rest - addition
    return np.array(holding)


def normal_values(key, extent, deviation, most, pieces=(), kind=jnp.bfloat16):
    level = levels(key, extent, pieces, -0.22, 0.18) if pieces else 1.0
    array = jax.random.normal(key, extent, jnp.float32) * deviation * level
    return jnp.minimum(jnp.maximum(array, -most), most).astype(kind)


def setup_inputs(seed: int = 0) -> dict:
    seeds = jax.random.split(jax.random.key(seed), 8)
    tokens = normal_values(seeds[0], (TOKENS, D), 1.0, 6.0, ((0, 24),))
    norm_gain = jnp.clip(1.0 + 0.18 * jax.random.normal(seeds[1], (D,), jnp.float32), 0.1, 1.9)
    route_ids_keys = jax.random.split(jax.random.fold_in(seeds[2], 1), TOKENS // TOK_DEV)
    route_ids_turns = jax.random.permutation(jax.random.fold_in(seeds[2], 3), TOKENS // TOK_DEV)
    route_ids = jax.vmap(lambda own, number: assign_block(jax.random.fold_in(seeds[2], 2), own, number, TOK_DEV, EXPERTS, TOPK, CAP, 2))(route_ids_keys, route_ids_turns).reshape((TOKENS, TOPK))
    route_weights = jnp.clip(jnp.exp(math.log(1.0) - 2.9957323 * jax.random.uniform(seeds[3], (TOKENS, TOPK), jnp.float32) ** levels(seeds[3], (TOKENS, TOPK), ((0, 24),), -0.2, 0.2)), 0.05, 1.0)
    gate_proj = normal_values(seeds[4], (EXPERTS, D, FF), D ** -0.5, 0.125, ((0, 24), (2, 32)))
    up_proj = normal_values(seeds[5], (EXPERTS, D, FF), D ** -0.5, 0.125, ((0, 24), (2, 32)))
    down_proj = normal_values(seeds[6], (EXPERTS, FF, D), FF ** -0.5, 0.0546875, ((0, 24), (1, 32)))
    return dict(tokens=tokens, norm_gain=norm_gain, route_ids=route_ids, route_weights=route_weights, gate_proj=gate_proj, up_proj=up_proj, down_proj=down_proj)


def reference(tokens, norm_gain, route_ids, route_weights, gate_proj, up_proj, down_proj):
    values = tokens.astype(jnp.float32)
    mean_square = lax.optimization_barrier(jnp.mean(values * values, axis=-1, keepdims=True))
    normed = (values * lax.rsqrt(mean_square + 1e-06) * norm_gain).astype(jnp.bfloat16)
    route_flat = route_ids.reshape(N_EP, TOK_DEV * TOPK)
    onehot = (route_flat[:, :, None] == jnp.arange(EXPERTS, dtype=jnp.int32)[None, None, :]).astype(jnp.int32)
    earlier = jnp.cumsum(onehot, axis=1) - onehot
    slot_index = lax.optimization_barrier(jnp.sum(earlier * onehot, axis=-1)).astype(jnp.int32)
    source_ids = jnp.arange(N_EP, dtype=jnp.int32)[:, None]
    buffer_row = (source_ids * CAP + slot_index).reshape(-1)
    expert_ids = route_flat.reshape(-1)
    repeated = jnp.repeat(normed, TOPK, axis=0)
    buffers = jnp.zeros((EXPERTS, N_EP * CAP, D), jnp.bfloat16).at[expert_ids, buffer_row].set(repeated)

    def expert(operands):
        rows_in, gate_w, up_w, down_w = operands
        gate_act = jnp.dot(rows_in, gate_w, preferred_element_type=jnp.float32)
        up_act = jnp.dot(rows_in, up_w, preferred_element_type=jnp.float32)
        hidden = (jax.nn.silu(gate_act) * up_act).astype(jnp.bfloat16)
        hidden_blocks = hidden.reshape(N_EP * CAP, N_TP, HID_BLOCK).astype(jnp.float32)
        down_blocks = down_w.reshape(N_TP, HID_BLOCK, D).astype(jnp.float32)
        partial_value = jnp.einsum('rbf,bfd->brd', hidden_blocks, down_blocks).astype(jnp.bfloat16)
        partial_value = lax.optimization_barrier(partial_value)
        return lax.optimization_barrier(jnp.sum(partial_value.astype(jnp.float32), axis=0))
    results = lax.map(expert, (buffers, gate_proj, up_proj, down_proj))
    picked = results[expert_ids, buffer_row].reshape(TOKENS, TOPK, D)
    mixed = lax.optimization_barrier(jnp.sum(route_weights[:, :, None] * picked, axis=1))
    return mixed.astype(jnp.bfloat16)
```

```python
import jax
import jax.numpy as jnp
from jax import lax
from jax.experimental import pallas as pl
from jax.experimental.pallas import tpu as pltpu
from jax.sharding import PartitionSpec as P

MESH = pl.DeviceIdType.MESH
NZ, NY, NX = 12, 8, 4
BF, F32 = jnp.bfloat16, jnp.float32
OFF = [0, 1, -1, 2, -2, 3, -3, 4, -4, 5, -5, 6]
GA, GB = (1, 5, 3), (6, 6, 3)
RA, RB = (7, 5, 3), (0, 7, 4)
DYS = [4, 3, -3, 2, -2, 1, -1, 0]
DXS = [2, 1, -1, 0]
WAYS = (1, -1)
N_SEND, N_TAKE = 224, 200


def part(span, way):
    start, count, cut = span
    return (start, cut) if way > 0 else (start + cut, count - cut)


def kernel(
    tok, gain, ids, wts, wg, wu, wd, out,
    x_buf, normed, z_out, near_out, wgu, wdn, acc, y_buf, comb_hi, comb_lo,
    ra_y, sa_y, za, ra_x, sa_x, rb_x, sb_x, zb, rb_y, sb_y, res, back,
    w_sem, s_sem, r_sem, b_sem,
):
    ep, tp = lax.axis_index("ep"), lax.axis_index("tp")
    z, core = lax.div(ep, 2), lax.rem(ep, 2)
    y, x = lax.div(tp, NX), lax.rem(tp, NX)
    half = lax.rem(x, 2)
    twin = tp + 1 - 2 * half

    def ym(d):
        return lax.rem(y + d + NY, NY)

    def xm(d):
        return lax.rem(x + d + NX, NX)

    def zm(d):
        return lax.rem(z + d + NZ, NZ)

    def tp_y(d):
        return ym(d) * NX + x

    def tp_x(d):
        return y * NX + xm(d)

    loads = [
        pltpu.make_async_copy(wg.at[0], wgu.at[:, pl.ds(0, 384)], w_sem.at[0]),
        pltpu.make_async_copy(wu.at[0], wgu.at[:, pl.ds(384, 384)], w_sem.at[1]),
        pltpu.make_async_copy(wd.at[0], wdn, w_sem.at[2]),
    ]
    for load in loads:
        load.start()

    barrier = pltpu.get_barrier_semaphore()

    def greet(e, t):
        pl.semaphore_signal(
            barrier, inc=1, device_id=(e, t), device_id_type=MESH
        )

    for off in OFF:
        for c in range(2):
            greet(2 * zm(off) + c, twin)
            if off != 0:
                greet(2 * zm(off) + c, tp)
    greet(2 * z + 1 - core, tp)
    for d in WAYS:
        greet(ep, tp_y(d))
    greet(ep, tp_x(2 * half - 1))

    send_places, take_places = {}, {}
    sent, sent_z = [], []

    def place(places, key):
        return places.setdefault(key, len(places))

    def arrival(key):
        return r_sem.at[place(take_places, key)]

    def message(key, src, dst, e, t, got=None):
        return pltpu.make_async_remote_copy(
            src_ref=src,
            dst_ref=dst,
            send_sem=s_sem.at[place(send_places, key)],
            recv_sem=arrival(key) if got is None else got,
            device_id=(e, t),
            device_id_type=MESH,
        )

    def send(*what):
        copy = message(*what)
        copy.start()
        sent.append(copy)

    def take(key, dst, got=None):
        pltpu.make_async_remote_copy(
            src_ref=dst,
            dst_ref=dst,
            send_sem=s_sem.at[0],
            recv_sem=arrival(key) if got is None else got,
            device_id=(ep, twin),
            device_id_type=MESH,
        ).wait_recv()

    def back_take(p, c):
        take(None, back.at[p, c], b_sem.at[2 * p + c])

    def norm_rows(i, carry):
        rows = pl.ds(pl.multiple_of(i * 16, 16), 16)
        values = tok[rows, :].astype(F32)
        mean = jnp.mean(values * values, axis=-1, keepdims=True)
        normed[rows, :] = (values * lax.rsqrt(mean + 1e-06) * gain[...]).astype(BF)
        return carry

    lax.fori_loop(0, 8, norm_rows, 0)

    lanes = lax.broadcasted_iota(jnp.int32, (128, 128), 1)
    rows = lax.broadcasted_iota(jnp.int32, (128, 128), 0)
    earlier = (rows < lanes).astype(F32).astype(BF)
    expert = lax.broadcasted_iota(jnp.int32, (32, 128), 0)
    id_rows = [ids[0:1, :], ids[1:2, :]]
    named = [(r == expert).astype(F32) for r in id_rows]
    before = jnp.dot((named[0] + named[1]).astype(BF), earlier, preferred_element_type=F32)
    pos = []
    for r, n in zip(id_rows, named):
        slot = jnp.sum(n * before, axis=0, keepdims=True).astype(jnp.int32)
        d = z - lax.shift_right_logical(r, 1)
        d = jnp.where(d < 0, d + NZ, d)
        tile = jnp.where(d == 0, 0, jnp.where(d <= 6, 2 * d - 1, 2 * (NZ - d)))
        pos.append(tile * 32 + (r & 1) * 16 + slot)
    row = lax.broadcasted_iota(jnp.int32, (384, 128), 0)
    at = [(p == row) for p in pos]
    pick = (at[0] | at[1]).astype(F32).astype(BF)

    column = pl.ds(pl.multiple_of(lax.div(tp, 2) * 128, 128), 128)
    rows_out = jnp.dot(pick, normed[:, column], preferred_element_type=F32)
    z_out[...] = rows_out.astype(BF).reshape(NZ, 2, 16, 128)

    pl.semaphore_wait(barrier, 24 + 22 + 1 + 2 + 1)

    for p in range(11, 0, -1):
        for c in range(2):
            sent_z.append(
                message(("z", p, c), z_out.at[p, c], x_buf.at[y, x, p],
                        2 * zm(-OFF[p]) + c, tp, arrival(("z", p)))
            )

    @pl.when(core == half)
    def _():
        for copy in sent_z:
            copy.start()

    row16 = lax.broadcasted_iota(jnp.int32, (16, 128), 0)
    for c in range(2):
        whose = core if c == 0 else 1 - core
        mine = ((pos[0] == row16 + whose * 16) | (pos[1] == row16 + whose * 16))
        near = jnp.dot(mine.astype(F32).astype(BF), normed[...], preferred_element_type=F32)
        near = near.astype(BF)
        for t in range(16):
            tile = near[:, t * 128 : (t + 1) * 128]
            if c == 0:
                x_buf[t // 2, 2 * (t % 2) + core, 0] = tile
            else:
                near_out[t % 2, t // 2] = tile
    for i in range(2):
        send(("near", i), near_out.at[i], x_buf.at[:, 2 * i + core, 0], 2 * z + 1 - core, tp)

    comb = jnp.where(at[0], wts[0:1, :], 0.0) + jnp.where(at[1], wts[1:2, :], 0.0)
    comb = jnp.transpose(comb)
    high = comb.astype(BF)
    comb_hi[...] = high
    comb_lo[...] = (comb - high.astype(F32)).astype(BF)

    def tiles(yy, xx, span):
        return x_buf.at[yy, xx, pl.ds(span[0], span[1])]

    def z_take(span):
        for p in range(span[0], span[0] + span[1]):
            take(("z", p), x_buf.at[y, x, p])

    def gax(step):
        for w in WAYS:
            if step == 1:
                send(("ax1", w), tiles(y, x, GA), tiles(y, x, GA), ep, tp_x(w))
            else:
                take(("ax1", w), tiles(y, xm(-w), GA))
                s = part(GA, w)
                send(("ax2", w), tiles(y, xm(-w), s), tiles(y, xm(-w), s), ep, tp_x(w))

    def gax_end():
        for w in WAYS:
            take(("ax2", w), tiles(y, xm(2), part(GA, w)))

    def gay(step, dx):
        xx = xm(dx)
        for w in WAYS:
            if step > 1:
                take(("ay", step - 1, dx, w), tiles(ym(-w * (step - 1)), xx, GA))
            s = part(GA, w) if step == 4 else GA
            src = tiles(ym(-w * (step - 1)), xx, s)
            send(("ay", step, dx, w), src, src, ep, tp_y(w))

    def gay_end(dx):
        for w in WAYS:
            take(("ay", 4, dx, w), tiles(ym(4), xm(dx), part(GA, w)))

    def gby(step):
        for w in WAYS:
            if step > 1:
                take(("by", step - 1, w), tiles(ym(-w * (step - 1)), x, GB))
            s = part(GB, w) if step == 4 else GB
            src = tiles(ym(-w * (step - 1)), x, s)
            send(("by", step, w), src, src, ep, tp_y(w))

    def gby_end():
        for w in WAYS:
            take(("by", 4, w), tiles(ym(4), x, part(GB, w)))

    def gbx(step, dy):
        yy = ym(dy)
        for w in WAYS:
            if step == 1:
                send(("bx1", dy, w), tiles(yy, x, GB), tiles(yy, x, GB), ep, tp_x(w))
            elif step == 2:
                take(("bx1", dy, w), tiles(yy, xm(-w), GB))
                s = part(GB, w)
                src = tiles(yy, xm(-w), s)
                send(("bx2", dy, w), src, src, ep, tp_x(w))
            else:
                take(("bx2", dy, w), tiles(yy, xm(2), part(GB, w)))

    def up(dy):
        yy = ym(dy)
        weights = wgu[pl.ds(pl.multiple_of(yy * 256, 256), 256), :]
        left = jnp.concatenate(
            [
                jnp.concatenate(
                    [x_buf[yy, h].reshape(192, 128), x_buf[yy, 2 + h].reshape(192, 128)],
                    axis=1,
                )
                for h in range(2)
            ],
            axis=0,
        )
        term = jnp.dot(left, weights, preferred_element_type=F32)
        acc[...] = term if dy == 0 else acc[...] + term

    z_take(GA)
    gax(1)
    gay(1, 0)
    gax(2)
    gay(1, 1)
    gay(1, -1)
    z_take(GB)
    gby(1)
    gbx(1, 0)
    gay(2, 0)
    gax_end()
    gay(1, 2)
    gay(2, 1)
    gay(2, -1)
    gby(2)
    gbx(2, 0)
    gbx(1, 1)
    gbx(1, -1)
    gay(3, 0)
    gay(2, 2)
    gay(3, 1)
    gay(3, -1)
    gby(3)
    gbx(3, 0)
    gbx(2, 1)
    gbx(2, -1)
    gbx(1, 2)
    gbx(1, -2)
    gay(4, 0)
    gay(3, 2)
    for i in range(2):
        take(("near", i), x_buf.at[:, 2 * i + 1 - core, 0])
    loads[0].wait()
    loads[1].wait()
    up(0)
    gby(4)
    gay(4, 1)
    gay(4, -1)
    gbx(3, 1)
    gbx(3, -1)
    gbx(2, 2)
    gbx(2, -2)
    gbx(1, 3)
    gbx(1, -3)
    gay(4, 2)
    gby_end()
    gbx(1, 4)
    up(1)
    up(-1)
    gbx(2, 3)
    gbx(2, -3)
    gbx(3, 2)
    gbx(3, -2)
    up(2)
    gbx(2, 4)
    up(-2)
    gbx(3, 3)
    gbx(3, -3)
    up(3)
    up(-3)
    for dx in (0, 1, -1, 2):
        gay_end(dx)
    gbx(3, 4)
    up(4)

    gate, upv = acc[:, :384], acc[:, 384:]
    hidden = (gate / (1.0 + jnp.exp(-gate)) * upv).astype(BF)
    loads[2].wait()

    def down(dy):
        yy = ym(dy)
        cols = pl.ds(pl.multiple_of(yy * 256, 256), 256)
        term = jnp.dot(hidden, wdn[:, cols], preferred_element_type=F32).astype(BF)
        for xx in range(NX):
            h, t = xx % 2, xx // 2
            block = term[192 * h : 192 * (h + 1), 128 * t : 128 * (t + 1)]
            y_buf[yy, xx] = block.reshape(NZ, 16, 128)

    def own(yy, xx, span):
        return y_buf[yy, xx, pl.ds(span[0], span[1])].astype(F32)

    def local(span, w):
        s = part(span, w)
        return pl.ds(s[0] - span[0], s[1])

    def whole(span):
        return pl.ds(0, span[1])

    def other(span, w):
        return local(span, -w)

    def ray(step):
        for dx in DXS:
            i = DXS.index(dx)
            for w in WAYS:
                d = 0 if w > 0 else 1
                yy = ym(w * (5 - step))
                if step == 1:
                    src = y_buf.at[yy, xm(dx), pl.ds(*part(RA, w))]
                    send(("ray", 1, dx, w), src, ra_y.at[d, 0, i, local(RA, w)], ep, tp_y(w))
                    continue
                if step == 2:
                    got = ra_y.at[d, 0, i, local(RA, w)]
                    take(("ray", 1, dx, w), got)
                    sa_y[d, 0, i, local(RA, w)] = (own(yy, xm(dx), part(RA, w)) + got[...].astype(F32)).astype(BF)
                    sa_y[d, 0, i, other(RA, w)] = y_buf[yy, xm(dx), pl.ds(*part(RA, -w))]
                else:
                    got = ra_y.at[d, step - 2, i]
                    take(("ray", step - 1, dx, w), got)
                    sa_y[d, step - 2, i] = (own(yy, xm(dx), RA) + got[...].astype(F32)).astype(BF)
                send(("ray", step, dx, w), sa_y.at[d, step - 2, i], ra_y.at[d, step - 1, i], ep, tp_y(w))

    def ray_end(dx):
        i = DXS.index(dx)
        total = own(y, xm(dx), RA)
        for w in WAYS:
            d = 0 if w > 0 else 1
            take(("ray", 4, dx, w), ra_y.at[d, 3, i])
            total = total + ra_y[d, 3, i].astype(F32)
        za[i] = total.astype(BF)

    def rax(step):
        for w in WAYS:
            d = 0 if w > 0 else 1
            here = local(RA, w)
            if step == 1:
                send(("rax", 1, w), za.at[0, here], ra_x.at[d, 0, here], ep, tp_x(w))
            else:
                got = ra_x.at[d, 0, here]
                take(("rax", 1, w), got)
                i = DXS.index(w)
                sa_x[d, here] = (za[i, here].astype(F32) + got[...].astype(F32)).astype(BF)
                sa_x[d, other(RA, w)] = za[i, other(RA, w)]
                send(("rax", 2, w), sa_x.at[d], ra_x.at[d, 1], ep, tp_x(w))

    def rax_end():
        total = za[3].astype(F32)
        for w in WAYS:
            d = 0 if w > 0 else 1
            take(("rax", 2, w), ra_x.at[d, 1])
            total = total + ra_x[d, 1].astype(F32)
        res[pl.ds(RA[0], RA[1])] = total.astype(BF)

    def rbx(step, dy):
        i, yy = DYS.index(dy), ym(dy)
        for w in WAYS:
            d = 0 if w > 0 else 1
            here = local(RB, w)
            if step == 1:
                src = y_buf.at[yy, xm(2), pl.ds(*part(RB, w))]
                send(("rbx", 1, dy, w), src, rb_x.at[i, d, 0, here], ep, tp_x(w))
            elif step == 2:
                got = rb_x.at[i, d, 0, here]
                take(("rbx", 1, dy, w), got)
                sb_x[i, d, here] = (own(yy, xm(w), part(RB, w)) + got[...].astype(F32)).astype(BF)
                sb_x[i, d, other(RB, w)] = y_buf[yy, xm(w), pl.ds(*part(RB, -w))]
                send(("rbx", 2, dy, w), sb_x.at[i, d], rb_x.at[i, d, 1], ep, tp_x(w))
        if step == 3:
            total = own(yy, x, RB)
            for w in WAYS:
                d = 0 if w > 0 else 1
                take(("rbx", 2, dy, w), rb_x.at[i, d, 1])
                total = total + rb_x[i, d, 1].astype(F32)
            zb[i] = total.astype(BF)

    def rby(step):
        for w in WAYS:
            d = 0 if w > 0 else 1
            here = local(RB, w)
            if step == 1:
                send(("rby", 1, w), zb.at[0, here], rb_y.at[d, 0, here], ep, tp_y(w))
                continue
            i = DYS.index(w * (5 - step))
            if step == 2:
                got = rb_y.at[d, 0, here]
                take(("rby", 1, w), got)
                sb_y[d, 0, here] = (zb[i, here].astype(F32) + got[...].astype(F32)).astype(BF)
                sb_y[d, 0, other(RB, w)] = zb[i, other(RB, w)]
            else:
                take(("rby", step - 1, w), rb_y.at[d, step - 2])
                sb_y[d, step - 2] = (zb[i].astype(F32) + rb_y[d, step - 2].astype(F32)).astype(BF)
            send(("rby", step, w), sb_y.at[d, step - 2], rb_y.at[d, step - 1], ep, tp_y(w))

    def rby_end():
        total = zb[7].astype(F32)
        for w in WAYS:
            d = 0 if w > 0 else 1
            take(("rby", 4, w), rb_y.at[d, 3])
            total = total + rb_y[d, 3].astype(F32)
        res[pl.ds(RB[0], RB[1])] = total.astype(BF)

    for dy in DYS:
        down(dy)
        if dy == 4:
            ray(1)
        rbx(1, dy)
    ray(2)
    for dy in DYS[:3]:
        rbx(2, dy)
    ray(3)
    for dy in DYS[3:]:
        rbx(2, dy)
    rbx(3, 4)
    rby(1)
    ray(4)
    rbx(3, 3)
    rbx(3, -3)
    rby(2)
    ray_end(2)
    rax(1)
    ray_end(1)
    ray_end(-1)
    rbx(3, 2)
    rbx(3, -2)
    rby(3)
    rax(2)
    ray_end(0)
    rbx(3, 1)
    rbx(3, -1)
    rby(4)

    def give(span):
        for p in range(span[0] + span[1] - 1, span[0] - 1, -1):
            e, got = 2 * zm(OFF[p]) + half, b_sem.at[2 * p + core]
            send(("back", p, 1), res.at[p], back.at[p, core], e, twin, got)
            if p > 0:
                send(("back", p, 0), res.at[p], back.at[p, core], e, tp, got)

    rax_end()
    give(RA)
    rbx(3, 0)
    rby_end()
    give(RB)
    near_back = message(
        ("back", 0, 0), res.at[0], back.at[0, core], 2 * z + half, tp, b_sem.at[core]
    )

    @pl.when(half == core)
    def _():
        back[0, core] = res[0]

    @pl.when(half != core)
    def _():
        near_back.start()

    for p in range(11, 0, -1):
        for c in range(2):
            back_take(p, c)
    back_take(0, 1 - core)

    @pl.when(half != core)
    def _():
        back_take(0, core)
        near_back.wait_send()

    rows_in = back[...].reshape(384, 128)
    mixed = jnp.dot(comb_hi[...], rows_in, preferred_element_type=F32)
    mixed = mixed + jnp.dot(comb_lo[...], rows_in, preferred_element_type=F32)
    mixed = jnp.where(half == 1, pltpu.roll(mixed, 64, 1), mixed)
    out[...] = mixed[:, :64].astype(BF)

    for copy in sent:
        copy.wait_send()

    @pl.when(core == half)
    def _():
        for copy in sent_z:
            copy.wait_send()


def per_device(tokens, norm_gain, route_ids, route_weights, gate_proj, up_proj, down_proj):
    vmem = pl.BlockSpec(memory_space=pltpu.VMEM)
    hbm = pl.BlockSpec(memory_space=pl.ANY)

    def tiles(*lead):
        return pltpu.VMEM((*lead, 16, 128), BF)

    a, b = RA[1], RB[1]
    return pl.pallas_call(
        kernel,
        out_shape=jax.ShapeDtypeStruct((128, 64), BF),
        in_specs=[vmem] * 4 + [hbm] * 3,
        out_specs=vmem,
        scratch_shapes=[
            tiles(NY, NX, NZ),
            pltpu.VMEM((128, 2048), BF),
            tiles(NZ, 2),
            tiles(2, NY),
            pltpu.VMEM((2048, 768), BF),
            pltpu.VMEM((384, 2048), BF),
            pltpu.VMEM((384, 768), F32),
            tiles(NY, NX, NZ),
            pltpu.VMEM((128, 384), BF),
            pltpu.VMEM((128, 384), BF),
            tiles(2, 4, 4, a), tiles(2, 3, 4, a), tiles(4, a), tiles(2, 2, a), tiles(2, a),
            tiles(8, 2, 2, b), tiles(8, 2, b), tiles(8, b), tiles(2, 4, b), tiles(2, 3, b),
            tiles(NZ),
            tiles(NZ, 2),
            pltpu.SemaphoreType.DMA((3,)),
            pltpu.SemaphoreType.DMA((N_SEND,)),
            pltpu.SemaphoreType.DMA((N_TAKE,)),
            pltpu.SemaphoreType.DMA((2 * NZ,)),
        ],
        compiler_params=pltpu.CompilerParams(collective_id=0, has_side_effects=True),
        cost_estimate=pl.CostEstimate(
            flops=2_000_000_000, bytes_accessed=6_000_000, transcendentals=200_000
        ),
    )(
        tokens, norm_gain.reshape(1, -1), route_ids.T, route_weights.T,
        gate_proj, up_proj, down_proj,
    )


def solution(mesh):
    placed = (
        P("ep", None),
        P(),
        P("ep", None),
        P("ep", None),
        P("ep", None, "tp"),
        P("ep", None, "tp"),
        P("ep", "tp", None),
    )
    return jax.shard_map(
        per_device, mesh=mesh, in_specs=placed, out_specs=P("ep", "tp"), check_vma=False
    )
```

```python
import jax
import jax.numpy as jnp
from jax import lax
from jax.experimental import pallas as pl
from jax.experimental.pallas import tpu as pltpu
from jax.sharding import PartitionSpec as P

MESH = pl.DeviceIdType.MESH
NZ, NY, NX = 12, 8, 4
BF, F32 = jnp.bfloat16, jnp.float32
OFF = [0, 1, -1, 2, -2, 3, -3, 4, -4, 5, -5, 6]
RA, RB = (0, 6, 3), (6, 6, 3)
NEAR = [(1, 2), (3, 2), (5, 1)]
FAR, LAST = (6, 3), (9, 3)
DYS = [4, 3, -3, 2, -2, 1, -1, 0]
DXS = [2, 1, -1, 0]
WAYS = (1, -1)
N_TAKE, POOL = 109, 2048


def part(span, way):
    start, count, cut = span
    return (start, cut) if way > 0 else (start + cut, count - cut)


def kernel(
    tok_in, gain_in, ids_in, wts_in, wg, wu, wd, out,
    tok, gain, ids, wts, x_buf, normed, z_near, z_far, near_out, wgu, wdn, acc, y_buf, comb_hi, comb_lo,
    ra_y, sa_y, za, ra_x, rb_x, sb_x, zb, rb_y, res, back,
    pool, w_sem, s_sem, r_sem,
):
    ep, tp = lax.axis_index("ep"), lax.axis_index("tp")
    z, core = lax.div(ep, 2), lax.rem(ep, 2)
    y, x = lax.div(tp, NX), lax.rem(tp, NX)
    half = lax.rem(x, 2)
    twin = tp + 1 - 2 * half

    def ym(d):
        return lax.rem(y + d + NY, NY)

    def xm(d):
        return lax.rem(x + d + NX, NX)

    def zm(d):
        return lax.rem(z + d + NZ, NZ)

    def tp_y(d):
        return ym(d) * NX + x

    def tp_x(d):
        return y * NX + xm(d)

    barrier = pltpu.get_barrier_semaphore()

    def greet(e, t):
        pl.semaphore_signal(barrier, inc=1, device_id=(e, t), device_id_type=MESH)

    for off in OFF[::-1]:
        for c in range(2):
            greet(2 * zm(off) + c, twin)
            if off != 0:
                greet(2 * zm(off) + c, tp)
    greet(2 * z + 1 - core, tp)
    for d in DYS[:-1]:
        greet(ep, tp_y(d))
    greet(ep, tp_x(2))
    greet(ep, tp_x(2 * half - 1))

    loads = [
        pltpu.make_async_copy(tok_in, tok, w_sem.at[0]),
        pltpu.make_async_copy(gain_in, gain, w_sem.at[1]),
        pltpu.make_async_copy(ids_in, ids, w_sem.at[2]),
        pltpu.make_async_copy(wts_in, wts, w_sem.at[3]),
        pltpu.make_async_copy(wg.at[0], wgu.at[:, pl.ds(0, 384)], w_sem.at[4]),
        pltpu.make_async_copy(wu.at[0], wgu.at[:, pl.ds(384, 384)], w_sem.at[5]),
        pltpu.make_async_copy(wd.at[0], wdn, w_sem.at[6]),
    ]
    for load in loads:
        load.start()

    places = {}
    sent, sent_z = [], []

    def arrival(key):
        return r_sem.at[places.setdefault(key, len(places))]

    def message(key, src, dst, e, t, group=0):
        return pltpu.make_async_remote_copy(
            src_ref=src,
            dst_ref=dst,
            send_sem=s_sem.at[group],
            recv_sem=arrival(key),
            device_id=(e, t),
            device_id_type=MESH,
        )

    def count(ref):
        size = 1
        for n in ref.shape:
            size *= n
        return size // 2048

    def send(key, src, dst, e, t):
        message(key, src, dst, e, t).start()
        sent.append(count(src))

    def take(key, dst):
        pltpu.make_async_remote_copy(
            src_ref=dst,
            dst_ref=dst,
            send_sem=s_sem.at[0],
            recv_sem=arrival(key),
            device_id=(ep, twin),
            device_id_type=MESH,
        ).wait_recv()

    def wait_sent(group, tiles):
        ref = pool.at[pl.ds(0, tiles)]
        pltpu.make_async_remote_copy(
            src_ref=ref,
            dst_ref=ref,
            send_sem=s_sem.at[group],
            recv_sem=r_sem.at[0],
            device_id=(ep, twin),
            device_id_type=MESH,
        ).wait_send()

    for load in loads[:4]:
        load.wait()

    def norm_rows(i, carry):
        rows = pl.ds(pl.multiple_of(i * 16, 16), 16)
        values = tok[rows, :].astype(F32)
        mean = jnp.mean(values * values, axis=-1, keepdims=True)
        normed[rows, :] = (values * lax.rsqrt(mean + 1e-06) * gain[...]).astype(BF)
        return carry

    lax.fori_loop(0, 8, norm_rows, 0)

    lanes = lax.broadcasted_iota(jnp.int32, (128, 128), 1)
    rows = lax.broadcasted_iota(jnp.int32, (128, 128), 0)
    earlier = (rows < lanes).astype(F32).astype(BF)
    expert = lax.broadcasted_iota(jnp.int32, (32, 128), 0)
    id_rows = [ids[0:1, :], ids[1:2, :]]
    named = [(r == expert).astype(F32) for r in id_rows]
    before = jnp.dot((named[0] + named[1]).astype(BF), earlier, preferred_element_type=F32)
    pos = []
    for r, n in zip(id_rows, named):
        slot = jnp.sum(n * before, axis=0, keepdims=True).astype(jnp.int32)
        d = z - lax.shift_right_logical(r, 1)
        d = jnp.where(d < 0, d + NZ, d)
        tile = jnp.where(d == 0, 0, jnp.where(d <= 6, 2 * d - 1, 2 * (NZ - d)))
        pos.append(tile * 32 + (r & 1) * 16 + slot)
    row = lax.broadcasted_iota(jnp.int32, (384, 128), 0)
    at = [(p == row) for p in pos]
    pick = (at[0] | at[1]).astype(F32).astype(BF)

    pair = lax.div(x, 2)
    column = pl.ds(pl.multiple_of(y * 256, 256), 256)
    rows_out = jnp.dot(pick[32:192], normed[:, column], preferred_element_type=F32)
    for t in range(2):
        z_near[:, :, t] = rows_out[:, 128 * t : 128 * (t + 1)].astype(BF).reshape(5, 2, 16, 128)
    for yy in range(NY):
        column = pl.ds(pl.multiple_of((2 * yy + pair) * 128, 128), 128)
        rows_out = jnp.dot(pick[192:], normed[:, column], preferred_element_type=F32)
        z_far[:, :, yy] = rows_out.astype(BF).reshape(6, 2, 16, 128)

    pl.semaphore_wait(barrier, 24 + 22 + 1 + 7 + 2)

    for p in range(1, 6):
        for c in range(2):
            send(("zn", (p - 1) // 2), z_near.at[p - 1, c], x_buf.at[y, :, core, p],
                 2 * zm(-OFF[p]) + c, tp)
    for p in (11, 10, 9, 8, 7, 6):
        for c in range(2):
            src, dst = z_far.at[p - 6, c], x_buf.at[:, pair, half, p]
            if p >= LAST[0]:
                src, dst = z_far.at[p - 6, c, y], x_buf.at[y, pair, half, p]
            key = ("zl",) if p >= LAST[0] else ("zf",)
            sent_z.append((message(key, src, dst, 2 * zm(-OFF[p]) + c, tp, 1), count(src)))

    @pl.when(core == half)
    def _():
        for copy, _ in sent_z:
            copy.start()

    row16 = lax.broadcasted_iota(jnp.int32, (16, 128), 0)
    for c in range(2):
        whose = core if c == 0 else 1 - core
        mine = ((pos[0] == row16 + whose * 16) | (pos[1] == row16 + whose * 16))
        near = jnp.dot(mine.astype(F32).astype(BF), normed[...], preferred_element_type=F32)
        near = near.astype(BF)
        for t in range(16):
            tile = near[:, t * 128 : (t + 1) * 128]
            if c == 0:
                x_buf[t // 2, t % 2, core, 0] = tile
            else:
                near_out[t // 2, t % 2] = tile
    send(("near",), near_out, x_buf.at[:, :, core, 0], 2 * z + 1 - core, tp)

    comb = jnp.where(at[0], wts[0:1, :], 0.0) + jnp.where(at[1], wts[1:2, :], 0.0)
    comb = jnp.transpose(comb)
    high = comb.astype(BF)
    comb_hi[...] = high
    comb_lo[...] = (comb - high.astype(F32)).astype(BF)

    def gather_y(chunk, step):
        ps = pl.ds(*NEAR[chunk])
        if step == 1:
            take(("zn", chunk), x_buf.at[y, :, :, ps])
        if step == 5:
            take(("gy", chunk, 4), x_buf.at[ym(4), :, :, ps])
            return
        for w in WAYS:
            yy = ym(-w * (step - 1))
            if step > 1:
                take(("gy", chunk, step - 1, w), x_buf.at[yy, :, :, ps])
            src = x_buf.at[yy, :, :, ps]
            if step == 4:
                src = x_buf.at[yy, 0 if w > 0 else 1, :, ps]
            key = ("gy", chunk, step) if step == 4 else ("gy", chunk, step, w)
            send(key, src, src, ep, tp_y(w))

    def column_of(rows, xx, ps):
        return x_buf.at[rows, lax.div(xx, 2), lax.rem(xx, 2), ps]

    def gather_x(step):
        ps = pl.ds(*FAR)
        if step == 1:
            take(("zf",), x_buf.at[:, pair, half, ps])
        if step == 3:
            take(("gx", 2), column_of(pl.ds(0, 8), xm(2), ps))
            return
        for w in WAYS:
            part_y = pl.ds(0 if w > 0 else 4, 4)
            xx = xm(-w * (step - 1))
            rows = pl.ds(0, 8)
            if step == 2:
                take(("gx", 1, w), column_of(rows, xx, ps))
                rows = part_y
            src = column_of(rows, xx, ps)
            send(("gx", step, w) if step == 1 else ("gx", 2), src, src, ep, tp_x(w))

    def last_y():
        src = x_buf.at[y, pair, half, pl.ds(*LAST)]
        take(("zl",), src)
        for dy in DYS[:7]:
            send(("ly", dy), src, src, ep, tp_y(dy))

    def last_x(step, *dys):
        if step == 3:
            take(("lx2",), column_of(pl.ds(0, 8), xm(2), pl.ds(*LAST)))
        for dy in dys:
            yy, cut = ym(-dy), 1 + DYS.index(dy) % 2
            if step == 1 and dy:
                take(("ly", dy), x_buf.at[yy, pair, half, pl.ds(*LAST)])
            for w in WAYS:
                ps = pl.ds(*LAST)
                piece = pl.ds(*part((*LAST, cut), w))
                xx = xm(-w * (step - 1))
                if step == 2:
                    take(("lx1", dy, w), column_of(yy, xx, ps))
                    ps = piece
                src = column_of(yy, xx, ps)
                send(("lx1", dy, w) if step == 1 else ("lx2",), src, src, ep, tp_x(w))

    def up(yy, first, start):
        weights = wgu[pl.ds(pl.multiple_of(yy * 256, 256), 256), :]
        ps = pl.ds(first, 6)
        left = jnp.concatenate(
            [
                jnp.concatenate(
                    [x_buf[yy, t, h, ps].reshape(96, 128) for t in range(2)], axis=1
                )
                for h in range(2)
            ],
            axis=0,
        )
        term = jnp.dot(left, weights, preferred_element_type=F32)
        acc[...] = term if start else acc[...] + term

    def act():
        gate, upv = acc[:, :384], acc[:, 384:]
        return (gate / (1.0 + jnp.exp(-gate)) * upv).astype(BF)

    def down(hidden, dy, first):
        yy = ym(dy)
        cols = pl.ds(pl.multiple_of(yy * 256, 256), 256)
        term = jnp.dot(hidden, wdn[:, cols], preferred_element_type=F32).astype(BF)
        for xx in range(NX):
            h, t = xx % 2, xx // 2
            block = term[96 * h : 96 * (h + 1), 128 * t : 128 * (t + 1)]
            y_buf[yy, xx, pl.ds(first, 6)] = block.reshape(6, 16, 128)

    def own(yy, xx, span):
        return y_buf[yy, xx, pl.ds(span[0], span[1])].astype(F32)

    def local(span, w):
        s = part(span, w)
        return pl.ds(s[0] - span[0], s[1])

    def whole(span):
        return pl.ds(0, span[1])

    def other(span, w):
        return local(span, -w)

    def ray(step):
        for dx in DXS:
            i = DXS.index(dx)
            for w in WAYS:
                d = 0 if w > 0 else 1
                yy = ym(w * (5 - step))
                if step == 1:
                    src = y_buf.at[yy, xm(dx), pl.ds(*part(RA, w))]
                    send(("ray", 1, dx, w), src, ra_y.at[d, 0, i, local(RA, w)], ep, tp_y(w))
                    continue
                if step == 2:
                    got = ra_y.at[d, 0, i, local(RA, w)]
                    take(("ray", 1, dx, w), got)
                    sa_y[d, 0, i, local(RA, w)] = (own(yy, xm(dx), part(RA, w)) + got[...].astype(F32)).astype(BF)
                    sa_y[d, 0, i, other(RA, w)] = y_buf[yy, xm(dx), pl.ds(*part(RA, -w))]
                else:
                    got = ra_y.at[d, step - 2, i]
                    take(("ray", step - 1, dx, w), got)
                    sa_y[d, step - 2, i] = (own(yy, xm(dx), RA) + got[...].astype(F32)).astype(BF)
                key = ("ray", 4, dx) if step == 4 else ("ray", step, dx, w)
                send(key, sa_y.at[d, step - 2, i], ra_y.at[d, step - 1, i], ep, tp_y(w))

    def ray_end(dx):
        i = DXS.index(dx)
        take(("ray", 4, dx), ra_y.at[:, 3, i])
        total = own(y, xm(dx), RA) + ra_y[0, 3, i].astype(F32) + ra_y[1, 3, i].astype(F32)
        za[i] = total.astype(BF)

    def rax(dx):
        i = DXS.index(dx)
        send(("rax",), za.at[i], ra_x.at[i], ep, tp_x(dx))

    def rax_end():
        total = za[3].astype(F32)
        take(("rax",), ra_x)
        for i in range(3):
            total = total + ra_x[i].astype(F32)
        res[pl.ds(RA[0], RA[1])] = total.astype(BF)

    def rbx(step, dy):
        i, yy = DYS.index(dy), ym(dy)
        for w in WAYS:
            d = 0 if w > 0 else 1
            here = local(RB, w)
            if step == 1:
                src = y_buf.at[yy, xm(2), pl.ds(*part(RB, w))]
                send(("rbx", 1, dy, w), src, rb_x.at[i, d, 0, here], ep, tp_x(w))
            elif step == 2:
                got = rb_x.at[i, d, 0, here]
                take(("rbx", 1, dy, w), got)
                sb_x[i, d, here] = (own(yy, xm(w), part(RB, w)) + got[...].astype(F32)).astype(BF)
                sb_x[i, d, other(RB, w)] = y_buf[yy, xm(w), pl.ds(*part(RB, -w))]
                send(("rbx", 2, dy), sb_x.at[i, d], rb_x.at[i, d, 1], ep, tp_x(w))
        if step == 3:
            take(("rbx", 2, dy), rb_x.at[i, :, 1])
            total = own(yy, x, RB) + rb_x[i, 0, 1].astype(F32) + rb_x[i, 1, 1].astype(F32)
            zb[i] = total.astype(BF)

            if i < 7:
                send(("rby",), zb.at[i], rb_y.at[i], ep, tp_y(dy))

    def rby_end():
        total = zb[7].astype(F32)
        take(("rby",), rb_y)
        for i in range(7):
            total = total + rb_y[i].astype(F32)
        res[pl.ds(RB[0], RB[1])] = total.astype(BF)

    for chunk in range(3):
        gather_y(chunk, 1)
    last_y()
    last_x(1, 0)
    gather_y(0, 2)
    gather_x(1)
    gather_y(1, 2)
    gather_y(2, 2)
    gather_y(0, 3)
    last_x(1, 1, -1)
    gather_y(1, 3)
    gather_y(2, 3)
    last_x(1, 2, -2)
    gather_x(2)
    gather_y(0, 4)
    last_x(1, 3, -3, 4)
    last_x(2, 0, 1, -1)
    gather_y(1, 4)
    gather_y(2, 4)
    take(("near",), x_buf.at[:, :, 1 - core, 0])
    loads[4].wait()
    loads[5].wait()
    for dy in (0, 1, -1):
        up(ym(dy), 0, dy == 0)
    last_x(2, 2, -2)
    for dy in (2, -2, 3, -3):
        up(ym(dy), 0, False)
    last_x(2, 3, -3, 4)
    for chunk in range(3):
        gather_y(chunk, 5)
    up(ym(4), 0, False)
    hidden = act()
    loads[6].wait()
    for dy in DYS:
        down(hidden, dy, 0)
        if dy == 4:
            ray(1)
    gather_x(3)
    last_x(3)
    ray(2)
    for yy in range(NY):
        up(yy, 6, yy == 0)
    hidden = act()
    for dy in DYS:
        down(hidden, dy, 6)
        rbx(1, dy)
    ray(3)
    for dy in DYS:
        rbx(2, dy)
    for dy in DYS[:3]:
        rbx(3, dy)
    ray(4)
    for dy in DYS[3:]:
        rbx(3, dy)
    for dx in DXS:
        ray_end(dx)
        if dx:
            rax(dx)

    def give(span):
        for p in range(span[0] + span[1] - 1, span[0] - 1, -1):
            e = 2 * zm(OFF[p]) + half
            send(("back",), res.at[p], back.at[p, core], e, twin)
            if p > 0:
                send(("back",), res.at[p], back.at[p, core], e, tp)

    rax_end()
    give(RA)
    rby_end()
    give(RB)
    near_back = message(("back",), res.at[0], back.at[0, core], 2 * z + half, tp, 2)

    @pl.when(half == core)
    def _():
        back[0, core] = res[0]
        take(("back",), pool.at[pl.ds(0, 23)])

    @pl.when(half != core)
    def _():
        near_back.start()
        take(("back",), pool.at[pl.ds(0, 24)])
        wait_sent(2, 1)

    rows_in = back[...].reshape(384, 128)
    mixed = jnp.dot(comb_hi[...], rows_in, preferred_element_type=F32)
    mixed = mixed + jnp.dot(comb_lo[...], rows_in, preferred_element_type=F32)
    mixed = jnp.where(half == 1, pltpu.roll(mixed, 64, 1), mixed)
    out[...] = mixed[:, :64].astype(BF)

    wait_sent(0, sum(sent))

    @pl.when(core == half)
    def _():
        wait_sent(1, sum(n for _, n in sent_z))

    assert len(places) == N_TAKE and sum(sent) <= POOL, (len(places), sum(sent))


def per_device(tokens, norm_gain, route_ids, route_weights, gate_proj, up_proj, down_proj):
    vmem = pl.BlockSpec(memory_space=pltpu.VMEM)
    hbm = pl.BlockSpec(memory_space=pl.ANY)

    def tiles(*lead):
        return pltpu.VMEM((*lead, 16, 128), BF)

    a, b = RA[1], RB[1]
    return pl.pallas_call(
        kernel,
        out_shape=jax.ShapeDtypeStruct((128, 64), BF),
        in_specs=[hbm] * 7,
        out_specs=vmem,
        scratch_shapes=[
            pltpu.VMEM((128, 2048), BF),
            pltpu.VMEM((1, 2048), F32),
            pltpu.VMEM((2, 128), jnp.int32),
            pltpu.VMEM((2, 128), F32),
            tiles(NY, 2, 2, NZ),
            pltpu.VMEM((128, 2048), BF),
            tiles(5, 2, 2),
            tiles(6, 2, NY),
            tiles(NY, 2),
            pltpu.VMEM((2048, 768), BF),
            pltpu.VMEM((384, 2048), BF),
            pltpu.VMEM((192, 768), F32),
            tiles(NY, NX, NZ),
            pltpu.VMEM((128, 384), BF),
            pltpu.VMEM((128, 384), BF),
            tiles(2, 4, 4, a), tiles(2, 3, 4, a), tiles(4, a), tiles(3, a),
            tiles(8, 2, 2, b), tiles(8, 2, b), tiles(8, b), tiles(7, b),
            tiles(NZ),
            tiles(NZ, 2),
            tiles(POOL),
            pltpu.SemaphoreType.DMA((7,)),
            pltpu.SemaphoreType.DMA((3,)),
            pltpu.SemaphoreType.DMA((N_TAKE,)),
        ],
        compiler_params=pltpu.CompilerParams(collective_id=0, has_side_effects=True),
        cost_estimate=pl.CostEstimate(
            flops=2_000_000_000, bytes_accessed=6_000_000, transcendentals=200_000
        ),
    )(
        tokens, norm_gain.reshape(1, -1), route_ids.T, route_weights.T,
        gate_proj, up_proj, down_proj,
    )


def solution(mesh):
    placed = (
        P("ep", None),
        P(),
        P("ep", None),
        P("ep", None),
        P("ep", None, "tp"),
        P("ep", None, "tp"),
        P("ep", "tp", None),
    )
    return jax.shard_map(
        per_device, mesh=mesh, in_specs=placed, out_specs=P("ep", "tp"), check_vma=False
    )
```

```python
import jax
import jax.numpy as jnp
from jax import lax
from jax.experimental import pallas as pl
from jax.experimental.pallas import tpu as pltpu
from jax.sharding import PartitionSpec as P

MESH = pl.DeviceIdType.MESH
NZ, NY, NX = 12, 8, 4
BF, F32 = jnp.bfloat16, jnp.float32
OFF = [0, 1, -1, 2, -2, 3, -3, 4, -4, 5, -5, 6]
RA, RB = (0, 6, 3), (6, 6, 3)
NEAR = [(1, 2), (3, 2), (5, 1)]
FAR, LAST = (6, 3), (9, 3)
LEGS = {11: (3, 3), 9: (3, 2), 10: (-3, -2), 7: (2, 2), 8: (-2, -2)}
DYS = [4, 3, -3, 2, -2, 1, -1, 0]
DXS = [2, 1, -1, 0]
WAYS = (1, -1)
N_TAKE, POOL = 114, 2048


def part(span, way):
    start, count, cut = span
    return (start, cut) if way > 0 else (start + cut, count - cut)


def kernel(
    tok_in, gain_in, ids_in, wts_in, wg, wu, wd, out,
    tok, gain, ids, wts, x_buf, normed, z_near, z_far, mid_far, mid_last, near_out, wgu, wdn, acc, y_buf, comb_hi, comb_lo,
    ra_y, sa_y, za, ra_x, rb_x, sb_x, zb, rb_y, res, back,
    pool, w_sem, s_sem, r_sem,
):
    ep, tp = lax.axis_index("ep"), lax.axis_index("tp")
    z, core = lax.div(ep, 2), lax.rem(ep, 2)
    y, x = lax.div(tp, NX), lax.rem(tp, NX)
    half = lax.rem(x, 2)
    twin = tp + 1 - 2 * half

    def ym(d):
        return lax.rem(y + d + NY, NY)

    def xm(d):
        return lax.rem(x + d + NX, NX)

    def zm(d):
        return lax.rem(z + d + NZ, NZ)

    def tp_y(d):
        return ym(d) * NX + x

    def tp_x(d):
        return y * NX + xm(d)

    barrier = pltpu.get_barrier_semaphore()

    def greet(e, t):
        pl.semaphore_signal(barrier, inc=1, device_id=(e, t), device_id_type=MESH)

    for off in OFF[6:0:-1]:
        for c in range(2):
            greet(2 * zm(off) + c, tp)
    greet(2 * z + 1 - core, tp)
    for d in DYS[:-1]:
        greet(ep, tp_y(d))
    for d in DXS[:-1]:
        greet(ep, tp_x(d))

    loads = [
        pltpu.make_async_copy(tok_in, tok, w_sem.at[0]),
        pltpu.make_async_copy(gain_in, gain, w_sem.at[1]),
        pltpu.make_async_copy(ids_in, ids, w_sem.at[2]),
        pltpu.make_async_copy(wts_in, wts, w_sem.at[3]),
        pltpu.make_async_copy(wg.at[0], wgu.at[:, pl.ds(0, 384)], w_sem.at[4]),
        pltpu.make_async_copy(wu.at[0], wgu.at[:, pl.ds(384, 384)], w_sem.at[5]),
        pltpu.make_async_copy(wd.at[0], wdn, w_sem.at[6]),
    ]
    for load in loads:
        load.start()

    places = {}
    sent, sent_z = [], []

    def arrival(key):
        return r_sem.at[places.setdefault(key, len(places))]

    def message(key, src, dst, e, t, group=0):
        return pltpu.make_async_remote_copy(
            src_ref=src,
            dst_ref=dst,
            send_sem=s_sem.at[group],
            recv_sem=arrival(key),
            device_id=(e, t),
            device_id_type=MESH,
        )

    def count(ref):
        size = 1
        for n in ref.shape:
            size *= n
        return size // 2048

    def send(key, src, dst, e, t):
        message(key, src, dst, e, t).start()
        sent.append(count(src))

    def take(key, dst):
        pltpu.make_async_remote_copy(
            src_ref=dst,
            dst_ref=dst,
            send_sem=s_sem.at[0],
            recv_sem=arrival(key),
            device_id=(ep, twin),
            device_id_type=MESH,
        ).wait_recv()

    def wait_sent(group, tiles):
        ref = pool.at[pl.ds(0, tiles)]
        pltpu.make_async_remote_copy(
            src_ref=ref,
            dst_ref=ref,
            send_sem=s_sem.at[group],
            recv_sem=r_sem.at[0],
            device_id=(ep, twin),
            device_id_type=MESH,
        ).wait_send()

    loads[2].wait()
    loads[3].wait()

    lanes = lax.broadcasted_iota(jnp.int32, (128, 128), 1)
    rows = lax.broadcasted_iota(jnp.int32, (128, 128), 0)
    earlier = (rows < lanes).astype(F32).astype(BF)
    expert = lax.broadcasted_iota(jnp.int32, (32, 128), 0)
    id_rows = [ids[0:1, :], ids[1:2, :]]
    named = [(r == expert).astype(F32) for r in id_rows]
    before = jnp.dot((named[0] + named[1]).astype(BF), earlier, preferred_element_type=F32)
    pos = []
    for r, n in zip(id_rows, named):
        slot = jnp.sum(n * before, axis=0, keepdims=True).astype(jnp.int32)
        d = z - lax.shift_right_logical(r, 1)
        d = jnp.where(d < 0, d + NZ, d)
        tile = jnp.where(d == 0, 0, jnp.where(d <= 6, 2 * d - 1, 2 * (NZ - d)))
        pos.append(tile * 32 + (r & 1) * 16 + slot)
    row = lax.broadcasted_iota(jnp.int32, (384, 128), 0)
    at = [(p == row) for p in pos]
    pick = (at[0] | at[1]).astype(F32).astype(BF)

    loads[0].wait()
    loads[1].wait()

    def norm_rows(i, carry):
        rows = pl.ds(pl.multiple_of(i * 16, 16), 16)
        values = tok[rows, :].astype(F32)
        mean = jnp.mean(values * values, axis=-1, keepdims=True)
        normed[rows, :] = (values * lax.rsqrt(mean + 1e-06) * gain[...]).astype(BF)
        return carry

    lax.fori_loop(0, 8, norm_rows, 0)

    pair = lax.div(x, 2)
    column = pl.ds(pl.multiple_of(y * 256, 256), 256)
    rows_out = jnp.dot(pick[32:192], normed[:, column], preferred_element_type=F32)
    for t in range(2):
        z_near[:, :, t] = rows_out[:, 128 * t : 128 * (t + 1)].astype(BF).reshape(5, 2, 16, 128)
    for yy in range(NY):
        column = pl.ds(pl.multiple_of((2 * yy + pair) * 128, 128), 128)
        rows_out = jnp.dot(pick[192:], normed[:, column], preferred_element_type=F32)
        z_far[:, :, yy] = rows_out.astype(BF).reshape(6, 2, 16, 128)

    pl.semaphore_wait(barrier, 12 + 1 + 7 + 3)

    for p in range(1, 6):
        for c in range(2):
            send(("zn", (p - 1) // 2), z_near.at[p - 1, c], x_buf.at[y, :, core, p],
                 2 * zm(-OFF[p]) + c, tp)
    def landing(p):
        return x_buf.at[y, pair, half, p] if p >= LAST[0] else x_buf.at[:, pair, half, p]

    def middle(p):
        return mid_last.at[p - 9] if p >= LAST[0] else mid_far.at[p - 7]

    for p in (*LEGS, 6):
        for c in range(2):
            src = z_far.at[p - 6, c, y] if p >= LAST[0] else z_far.at[p - 6, c]
            if p in LEGS:
                copy = message(("mid", p), src, middle(p), 2 * zm(-LEGS[p][0]) + c, tp, 1)
            else:
                copy = message(("zf",), src, landing(p), 2 * zm(-OFF[p]) + c, tp, 1)
            sent_z.append((copy, count(src)))

    @pl.when(core == half)
    def _():
        for copy, _ in sent_z:
            copy.start()

    row16 = lax.broadcasted_iota(jnp.int32, (16, 128), 0)
    for c in range(2):
        whose = core if c == 0 else 1 - core
        mine = ((pos[0] == row16 + whose * 16) | (pos[1] == row16 + whose * 16))
        near = jnp.dot(mine.astype(F32).astype(BF), normed[...], preferred_element_type=F32)
        near = near.astype(BF)
        for t in range(16):
            tile = near[:, t * 128 : (t + 1) * 128]
            if c == 0:
                x_buf[t // 2, t % 2, core, 0] = tile
            else:
                near_out[t // 2, t % 2] = tile
    send(("near",), near_out, x_buf.at[:, :, core, 0], 2 * z + 1 - core, tp)

    comb = jnp.where(at[0], wts[0:1, :], 0.0) + jnp.where(at[1], wts[1:2, :], 0.0)
    comb = jnp.transpose(comb)
    high = comb.astype(BF)
    comb_hi[...] = high
    comb_lo[...] = (comb - high.astype(F32)).astype(BF)

    def hand_on(*tiles_held):
        for p in tiles_held:
            take(("mid", p), middle(p))
            key = ("zl",) if p >= LAST[0] else ("zf",)
            send(key, middle(p), landing(p), 2 * zm(-LEGS[p][1]) + core, tp)

    def gather_y(chunk, step):
        ps = pl.ds(*NEAR[chunk])
        if step == 1:
            take(("zn", chunk), x_buf.at[y, :, :, ps])
        if step == 5:
            take(("gy", chunk, 4), x_buf.at[ym(4), :, :, ps])
            return
        for w in WAYS:
            yy = ym(-w * (step - 1))
            if step > 1:
                take(("gy", chunk, step - 1, w), x_buf.at[yy, :, :, ps])
            src = x_buf.at[yy, :, :, ps]
            if step == 4:
                src = x_buf.at[yy, 0 if w > 0 else 1, :, ps]
            key = ("gy", chunk, step) if step == 4 else ("gy", chunk, step, w)
            send(key, src, src, ep, tp_y(w))

    def column_of(rows, xx, ps):
        return x_buf.at[rows, lax.div(xx, 2), lax.rem(xx, 2), ps]

    def gather_x(step):
        ps = pl.ds(*FAR)
        if step == 1:
            take(("zf",), x_buf.at[:, pair, half, ps])
        if step == 3:
            take(("gx", 2), column_of(pl.ds(0, 8), xm(2), ps))
            return
        for w in WAYS:
            part_y = pl.ds(0 if w > 0 else 4, 4)
            xx = xm(-w * (step - 1))
            rows = pl.ds(0, 8)
            if step == 2:
                take(("gx", 1, w), column_of(rows, xx, ps))
                rows = part_y
            src = column_of(rows, xx, ps)
            send(("gx", step, w) if step == 1 else ("gx", 2), src, src, ep, tp_x(w))

    def last_y():
        src = x_buf.at[y, pair, half, pl.ds(*LAST)]
        take(("zl",), src)
        for dy in DYS[:7]:
            send(("ly", dy), src, src, ep, tp_y(dy))

    def last_x(step, *dys):
        if step == 3:
            take(("lx2",), column_of(pl.ds(0, 8), xm(2), pl.ds(*LAST)))
        for dy in dys:
            yy, cut = ym(-dy), 1 + DYS.index(dy) % 2
            if step == 1 and dy:
                take(("ly", dy), x_buf.at[yy, pair, half, pl.ds(*LAST)])
            for w in WAYS:
                ps = pl.ds(*LAST)
                piece = pl.ds(*part((*LAST, cut), w))
                xx = xm(-w * (step - 1))
                if step == 2:
                    take(("lx1", dy, w), column_of(yy, xx, ps))
                    ps = piece
                src = column_of(yy, xx, ps)
                send(("lx1", dy, w) if step == 1 else ("lx2",), src, src, ep, tp_x(w))

    def up(yy, first, start):
        weights = wgu[pl.ds(pl.multiple_of(yy * 256, 256), 256), :]
        ps = pl.ds(first, 6)
        left = jnp.concatenate(
            [
                jnp.concatenate(
                    [x_buf[yy, t, h, ps].reshape(96, 128) for t in range(2)], axis=1
                )
                for h in range(2)
            ],
            axis=0,
        )
        term = jnp.dot(left, weights, preferred_element_type=F32)
        acc[...] = term if start else acc[...] + term

    def act():
        gate, upv = acc[:, :384], acc[:, 384:]
        return (gate / (1.0 + jnp.exp(-gate)) * upv).astype(BF)

    def down(hidden, dy, first):
        yy = ym(dy)
        cols = pl.ds(pl.multiple_of(yy * 256, 256), 256)
        term = jnp.dot(hidden, wdn[:, cols], preferred_element_type=F32).astype(BF)
        for xx in range(NX):
            h, t = xx % 2, xx // 2
            block = term[96 * h : 96 * (h + 1), 128 * t : 128 * (t + 1)]
            y_buf[yy, xx, pl.ds(first, 6)] = block.reshape(6, 16, 128)

    def own(yy, xx, span):
        return y_buf[yy, xx, pl.ds(span[0], span[1])].astype(F32)

    def local(span, w):
        s = part(span, w)
        return pl.ds(s[0] - span[0], s[1])

    def whole(span):
        return pl.ds(0, span[1])

    def other(span, w):
        return local(span, -w)

    def ray(step):
        for dx in DXS:
            i = DXS.index(dx)
            for w in WAYS:
                d = 0 if w > 0 else 1
                yy = ym(w * (5 - step))
                if step == 1:
                    src = y_buf.at[yy, xm(dx), pl.ds(*part(RA, w))]
                    send(("ray", 1, dx, w), src, ra_y.at[d, 0, i, local(RA, w)], ep, tp_y(w))
                    continue
                if step == 2:
                    got = ra_y.at[d, 0, i, local(RA, w)]
                    take(("ray", 1, dx, w), got)
                    sa_y[d, 0, i, local(RA, w)] = (own(yy, xm(dx), part(RA, w)) + got[...].astype(F32)).astype(BF)
                    sa_y[d, 0, i, other(RA, w)] = y_buf[yy, xm(dx), pl.ds(*part(RA, -w))]
                else:
                    got = ra_y.at[d, step - 2, i]
                    take(("ray", step - 1, dx, w), got)
                    sa_y[d, step - 2, i] = (own(yy, xm(dx), RA) + got[...].astype(F32)).astype(BF)
                key = ("ray", 4, dx) if step == 4 else ("ray", step, dx, w)
                send(key, sa_y.at[d, step - 2, i], ra_y.at[d, step - 1, i], ep, tp_y(w))

    def ray_end(dx):
        i = DXS.index(dx)
        take(("ray", 4, dx), ra_y.at[:, 3, i])
        total = own(y, xm(dx), RA) + ra_y[0, 3, i].astype(F32) + ra_y[1, 3, i].astype(F32)
        za[i] = total.astype(BF)

    def rax(dx):
        i = DXS.index(dx)
        send(("rax",), za.at[i], ra_x.at[i], ep, tp_x(dx))

    def rax_end():
        total = za[3].astype(F32)
        take(("rax",), ra_x)
        for i in range(3):
            total = total + ra_x[i].astype(F32)
        res[pl.ds(RA[0], RA[1])] = total.astype(BF)

    def rbx(step, dy):
        i, yy = DYS.index(dy), ym(dy)
        for w in WAYS:
            d = 0 if w > 0 else 1
            here = local(RB, w)
            if step == 1:
                src = y_buf.at[yy, xm(2), pl.ds(*part(RB, w))]
                send(("rbx", 1, dy, w), src, rb_x.at[i, d, 0, here], ep, tp_x(w))
            elif step == 2:
                got = rb_x.at[i, d, 0, here]
                take(("rbx", 1, dy, w), got)
                sb_x[i, d, here] = (own(yy, xm(w), part(RB, w)) + got[...].astype(F32)).astype(BF)
                sb_x[i, d, other(RB, w)] = y_buf[yy, xm(w), pl.ds(*part(RB, -w))]
                send(("rbx", 2, dy), sb_x.at[i, d], rb_x.at[i, d, 1], ep, tp_x(w))
        if step == 3:
            take(("rbx", 2, dy), rb_x.at[i, :, 1])
            total = own(yy, x, RB) + rb_x[i, 0, 1].astype(F32) + rb_x[i, 1, 1].astype(F32)
            zb[i] = total.astype(BF)

            if i < 7:
                send(("rby",), zb.at[i], rb_y.at[i], ep, tp_y(dy))

    def rby_end():
        total = zb[7].astype(F32)
        take(("rby",), rb_y)
        for i in range(7):
            total = total + rb_y[i].astype(F32)
        res[pl.ds(RB[0], RB[1])] = total.astype(BF)

    gather_y(0, 1)
    gather_y(1, 1)
    hand_on(*LEGS)
    gather_y(2, 1)
    gather_y(0, 2)
    gather_y(1, 2)
    last_y()
    last_x(1, 0)
    gather_y(2, 2)
    gather_x(1)
    gather_y(0, 3)
    gather_y(1, 3)
    last_x(1, 1, -1)
    gather_y(2, 3)
    gather_x(2)
    gather_y(0, 4)
    last_x(1, 2, -2)
    gather_y(1, 4)
    gather_y(2, 4)
    last_x(1, 3, -3, 4)
    take(("near",), x_buf.at[:, :, 1 - core, 0])
    loads[4].wait()
    loads[5].wait()
    for dy in (0, 1, -1):
        up(ym(dy), 0, dy == 0)
    last_x(2, 0, 1, -1)
    for dy in (2, -2):
        up(ym(dy), 0, False)
    last_x(2, 2, -2)
    for dy in (3, -3):
        up(ym(dy), 0, False)
    for chunk in range(3):
        gather_y(chunk, 5)
    up(ym(4), 0, False)
    hidden = act()
    loads[6].wait()
    down(hidden, 4, 0)
    ray(1)
    for dy in DYS[1:4]:
        down(hidden, dy, 0)
    last_x(2, 3, -3, 4)
    for dy in DYS[4:]:
        down(hidden, dy, 0)
    gather_x(3)
    ray(2)
    last_x(3)
    for yy in range(NY):
        up(yy, 6, yy == 0)
    hidden = act()
    for dy in DYS[:4]:
        down(hidden, dy, 6)
        rbx(1, dy)
    ray(3)
    for dy in DYS[4:]:
        down(hidden, dy, 6)
        rbx(1, dy)
    for dy in DYS[:3]:
        rbx(2, dy)
    ray(4)
    for dy in DYS[3:]:
        rbx(2, dy)
    for dy in DYS[:3]:
        rbx(3, dy)
    for dx in DXS[:3]:
        ray_end(dx)
        rax(dx)
    for dy in DYS[3:]:
        rbx(3, dy)
    ray_end(0)

    def give(span):
        for p in range(span[0] + span[1] - 1, span[0] - 1, -1):
            e = 2 * zm(OFF[p]) + half
            send(("back",), res.at[p], back.at[p, core], e, twin)
            if p > 0:
                send(("back",), res.at[p], back.at[p, core], e, tp)

    rax_end()
    give(RA)
    rby_end()
    give(RB)
    near_back = message(("back",), res.at[0], back.at[0, core], 2 * z + half, tp, 2)

    @pl.when(half == core)
    def _():
        back[0, core] = res[0]
        take(("back",), pool.at[pl.ds(0, 23)])

    @pl.when(half != core)
    def _():
        near_back.start()
        take(("back",), pool.at[pl.ds(0, 24)])
        wait_sent(2, 1)

    rows_in = back[...].reshape(384, 128)
    mixed = jnp.dot(comb_hi[...], rows_in, preferred_element_type=F32)
    mixed = mixed + jnp.dot(comb_lo[...], rows_in, preferred_element_type=F32)
    mixed = jnp.transpose(mixed)
    out[...] = jnp.where(half == 1, mixed[64:], mixed[:64]).astype(BF)

    wait_sent(0, sum(sent))

    @pl.when(core == half)
    def _():
        wait_sent(1, sum(n for _, n in sent_z))

    assert len(places) == N_TAKE and sum(sent) <= POOL, (len(places), sum(sent))


def per_device(tokens, norm_gain, route_ids, route_weights, gate_proj, up_proj, down_proj):
    vmem = pl.BlockSpec(memory_space=pltpu.VMEM)
    hbm = pl.BlockSpec(memory_space=pl.ANY)

    def tiles(*lead):
        return pltpu.VMEM((*lead, 16, 128), BF)

    a, b = RA[1], RB[1]
    return pl.pallas_call(
        kernel,
        out_shape=jax.ShapeDtypeStruct((64, 128), BF),
        in_specs=[hbm] * 7,
        out_specs=vmem,
        scratch_shapes=[
            pltpu.VMEM((128, 2048), BF),
            pltpu.VMEM((1, 2048), F32),
            pltpu.VMEM((2, 128), jnp.int32),
            pltpu.VMEM((2, 128), F32),
            tiles(NY, 2, 2, NZ),
            pltpu.VMEM((128, 2048), BF),
            tiles(5, 2, 2),
            tiles(6, 2, NY),
            tiles(2, NY),
            tiles(3),
            tiles(NY, 2),
            pltpu.VMEM((2048, 768), BF),
            pltpu.VMEM((384, 2048), BF),
            pltpu.VMEM((192, 768), F32),
            tiles(NY, NX, NZ),
            pltpu.VMEM((128, 384), BF),
            pltpu.VMEM((128, 384), BF),
            tiles(2, 4, 4, a), tiles(2, 3, 4, a), tiles(4, a), tiles(3, a),
            tiles(8, 2, 2, b), tiles(8, 2, b), tiles(8, b), tiles(7, b),
            tiles(NZ),
            tiles(NZ, 2),
            tiles(POOL),
            pltpu.SemaphoreType.DMA((7,)),
            pltpu.SemaphoreType.DMA((3,)),
            pltpu.SemaphoreType.DMA((N_TAKE,)),
        ],
        compiler_params=pltpu.CompilerParams(collective_id=0, has_side_effects=True),
        cost_estimate=pl.CostEstimate(
            flops=2_000_000_000, bytes_accessed=6_000_000, transcendentals=200_000
        ),
    )(
        tokens, norm_gain.reshape(1, -1), route_ids.T, route_weights.T,
        gate_proj, up_proj, down_proj,
    ).T


def solution(mesh):
    placed = (
        P("ep", None),
        P(),
        P("ep", None),
        P("ep", None),
        P("ep", None, "tp"),
        P("ep", None, "tp"),
        P("ep", "tp", None),
    )
    return jax.shard_map(
        per_device, mesh=mesh, in_specs=placed, out_specs=P("ep", "tp"), check_vma=False
    )
```

```python
import jax
import jax.numpy as jnp
from jax import lax
from jax.experimental import pallas as pl
from jax.experimental.pallas import tpu as pltpu
from jax.sharding import PartitionSpec as P

MESH = pl.DeviceIdType.MESH
NZ, NY, NX = 12, 8, 4
BF, F32 = jnp.bfloat16, jnp.float32
OFF = [0, 1, -1, 2, -2, 3, -3, 4, -4, 5, -5, 6]
RA, RB = (0, 6, 3), (6, 6, 3)
NEAR = [(1, 2), (3, 2), (5, 1)]
FAR, LAST = (6, 3), (9, 3)
LEGS = {11: (3, 3), 9: (3, 2), 10: (-3, -2), 7: (2, 2), 8: (-2, -2)}
DYS = [4, 3, -3, 2, -2, 1, -1, 0]
DXS = [2, 1, -1, 0]
WAYS = (1, -1)
N_TAKE, POOL = 114, 2048


def part(span, way):
    start, count, cut = span
    return (start, cut) if way > 0 else (start + cut, count - cut)


def kernel(
    tok_in, gain_in, ids_in, wts_in, wg, wu, wd, out,
    tok, gain, ids, wts, x_buf, normed, z_near, z_far, mid_far, mid_last, near_out, wgu, wdn, acc, y_buf, comb_hi, comb_lo,
    ra_y, sa_y, za, ra_x, rb_x, sb_x, zb, rb_y, res, back,
    pool, w_sem, s_sem, r_sem,
):
    ep, tp = lax.axis_index("ep"), lax.axis_index("tp")
    z, core = lax.div(ep, 2), lax.rem(ep, 2)
    y, x = lax.div(tp, NX), lax.rem(tp, NX)
    half = lax.rem(x, 2)
    twin = tp + 1 - 2 * half

    def ym(d):
        return lax.rem(y + d + NY, NY)

    def xm(d):
        return lax.rem(x + d + NX, NX)

    def zm(d):
        return lax.rem(z + d + NZ, NZ)

    def tp_y(d):
        return ym(d) * NX + x

    def tp_x(d):
        return y * NX + xm(d)

    barrier = pltpu.get_barrier_semaphore()

    def greet(e, t):
        pl.semaphore_signal(barrier, inc=1, device_id=(e, t), device_id_type=MESH)

    for off in OFF[6:0:-1]:
        for c in range(2):
            greet(2 * zm(off) + c, tp)
    greet(2 * z + 1 - core, tp)
    for d in DYS[3:-1]:
        greet(ep, tp_y(d))
    for d in DXS[:-1]:
        greet(ep, tp_x(d))

    loads = [
        pltpu.make_async_copy(tok_in, tok, w_sem.at[0]),
        pltpu.make_async_copy(gain_in, gain, w_sem.at[1]),
        pltpu.make_async_copy(ids_in, ids, w_sem.at[2]),
        pltpu.make_async_copy(wts_in, wts, w_sem.at[3]),
        pltpu.make_async_copy(wg.at[0], wgu.at[:, pl.ds(0, 384)], w_sem.at[4]),
        pltpu.make_async_copy(wu.at[0], wgu.at[:, pl.ds(384, 384)], w_sem.at[5]),
        pltpu.make_async_copy(wd.at[0], wdn, w_sem.at[6]),
    ]
    for load in loads:
        load.start()

    places = {}
    sent, sent_z = [], []

    def arrival(key):
        return r_sem.at[places.setdefault(key, len(places))]

    def message(key, src, dst, e, t, group=0):
        return pltpu.make_async_remote_copy(
            src_ref=src,
            dst_ref=dst,
            send_sem=s_sem.at[group],
            recv_sem=arrival(key),
            device_id=(e, t),
            device_id_type=MESH,
        )

    def count(ref):
        size = 1
        for n in ref.shape:
            size *= n
        return size // 2048

    def send(key, src, dst, e, t):
        message(key, src, dst, e, t).start()
        sent.append(count(src))

    def take(key, dst):
        pltpu.make_async_remote_copy(
            src_ref=dst,
            dst_ref=dst,
            send_sem=s_sem.at[0],
            recv_sem=arrival(key),
            device_id=(ep, twin),
            device_id_type=MESH,
        ).wait_recv()

    def wait_sent(group, tiles):
        ref = pool.at[pl.ds(0, tiles)]
        pltpu.make_async_remote_copy(
            src_ref=ref,
            dst_ref=ref,
            send_sem=s_sem.at[group],
            recv_sem=r_sem.at[0],
            device_id=(ep, twin),
            device_id_type=MESH,
        ).wait_send()

    loads[2].wait()
    loads[3].wait()

    lanes = lax.broadcasted_iota(jnp.int32, (128, 128), 1)
    rows = lax.broadcasted_iota(jnp.int32, (128, 128), 0)
    earlier = (rows < lanes).astype(F32).astype(BF)
    expert = lax.broadcasted_iota(jnp.int32, (32, 128), 0)
    id_rows = [ids[0:1, :], ids[1:2, :]]
    named = [(r == expert).astype(F32) for r in id_rows]
    before = jnp.dot((named[0] + named[1]).astype(BF), earlier, preferred_element_type=F32)
    pos = []
    for r, n in zip(id_rows, named):
        slot = jnp.sum(n * before, axis=0, keepdims=True).astype(jnp.int32)
        d = z - lax.shift_right_logical(r, 1)
        d = jnp.where(d < 0, d + NZ, d)
        tile = jnp.where(d == 0, 0, jnp.where(d <= 6, 2 * d - 1, 2 * (NZ - d)))
        pos.append(tile * 32 + (r & 1) * 16 + slot)
    row = lax.broadcasted_iota(jnp.int32, (384, 128), 0)
    at = [(p == row) for p in pos]
    pick = (at[0] | at[1]).astype(F32).astype(BF)

    loads[0].wait()
    loads[1].wait()

    def norm_rows(i, carry):
        rows = pl.ds(pl.multiple_of(i * 16, 16), 16)
        values = tok[rows, :].astype(F32)
        mean = jnp.mean(values * values, axis=-1, keepdims=True)
        normed[rows, :] = (values * lax.rsqrt(mean + 1e-06) * gain[...]).astype(BF)
        return carry

    lax.fori_loop(0, 8, norm_rows, 0)

    pair = lax.div(x, 2)
    column = pl.ds(pl.multiple_of(y * 256, 256), 256)
    rows_out = jnp.dot(pick[32:192], normed[:, column], preferred_element_type=F32)
    for t in range(2):
        z_near[:, :, t] = rows_out[:, 128 * t : 128 * (t + 1)].astype(BF).reshape(5, 2, 16, 128)
    for yy in range(NY):
        column = pl.ds(pl.multiple_of((2 * yy + pair) * 128, 128), 128)
        rows_out = jnp.dot(pick[192:], normed[:, column], preferred_element_type=F32)
        z_far[:, :, yy] = rows_out.astype(BF).reshape(6, 2, 16, 128)

    pl.semaphore_wait(barrier, 12 + 1 + 4 + 3)

    for p in range(1, 6):
        for c in range(2):
            send(("zn", (p - 1) // 2), z_near.at[p - 1, c], x_buf.at[y, :, core, p],
                 2 * zm(-OFF[p]) + c, tp)
    def landing(p):
        return x_buf.at[y, pair, half, p] if p >= LAST[0] else x_buf.at[:, pair, half, p]

    def middle(p):
        return mid_last.at[p - 9] if p >= LAST[0] else mid_far.at[p - 7]

    for p in (*LEGS, 6):
        for c in range(2):
            src = z_far.at[p - 6, c, y] if p >= LAST[0] else z_far.at[p - 6, c]
            if p in LEGS:
                copy = message(("mid", p), src, middle(p), 2 * zm(-LEGS[p][0]) + c, tp, 1)
            else:
                copy = message(("zf",), src, landing(p), 2 * zm(-OFF[p]) + c, tp, 1)
            sent_z.append((copy, count(src)))

    @pl.when(core == half)
    def _():
        for copy, _ in sent_z:
            copy.start()

    row16 = lax.broadcasted_iota(jnp.int32, (16, 128), 0)
    for c in range(2):
        whose = core if c == 0 else 1 - core
        mine = ((pos[0] == row16 + whose * 16) | (pos[1] == row16 + whose * 16))
        near = jnp.dot(mine.astype(F32).astype(BF), normed[...], preferred_element_type=F32)
        near = near.astype(BF)
        for t in range(16):
            tile = near[:, t * 128 : (t + 1) * 128]
            if c == 0:
                x_buf[t // 2, t % 2, core, 0] = tile
            else:
                near_out[t // 2, t % 2] = tile
    send(("near",), near_out, x_buf.at[:, :, core, 0], 2 * z + 1 - core, tp)

    comb = jnp.where(at[0], wts[0:1, :], 0.0) + jnp.where(at[1], wts[1:2, :], 0.0)
    comb = jnp.transpose(comb)
    high = comb.astype(BF)
    comb_hi[...] = high
    comb_lo[...] = (comb - high.astype(F32)).astype(BF)

    def hand_on(*tiles_held):
        for p in tiles_held:
            take(("mid", p), middle(p))
            key = ("zl",) if p >= LAST[0] else ("zf",)
            send(key, middle(p), landing(p), 2 * zm(-LEGS[p][1]) + core, tp)

    def gather_y(chunk, step):
        ps = pl.ds(*NEAR[chunk])
        if step == 1:
            take(("zn", chunk), x_buf.at[y, :, :, ps])
        if step == 5:
            take(("gy", chunk, 4), x_buf.at[ym(4), :, :, ps])
            return
        for w in WAYS:
            yy = ym(-w * (step - 1))
            if step > 1:
                take(("gy", chunk, step - 1, w), x_buf.at[yy, :, :, ps])
            src = x_buf.at[yy, :, :, ps]
            if step == 4:
                src = x_buf.at[yy, 0 if w > 0 else 1, :, ps]
            key = ("gy", chunk, step) if step == 4 else ("gy", chunk, step, w)
            send(key, src, src, ep, tp_y(w))

    def column_of(rows, xx, ps):
        return x_buf.at[rows, lax.div(xx, 2), lax.rem(xx, 2), ps]

    def gather_x(step):
        ps = pl.ds(*FAR)
        if step == 1:
            take(("zf",), x_buf.at[:, pair, half, ps])
        if step == 3:
            take(("gx", 2), column_of(pl.ds(0, 8), xm(2), ps))
            return
        for w in WAYS:
            part_y = pl.ds(0 if w > 0 else 4, 4)
            xx = xm(-w * (step - 1))
            rows = pl.ds(0, 8)
            if step == 2:
                take(("gx", 1, w), column_of(rows, xx, ps))
                rows = part_y
            src = column_of(rows, xx, ps)
            send(("gx", step, w) if step == 1 else ("gx", 2), src, src, ep, tp_x(w))

    def last_y(dys):
        src = x_buf.at[y, pair, half, pl.ds(*LAST)]
        if len(dys) > 1:
            take(("zl",), src)
        for dy in dys:
            send(("ly", dy), src, src, ep, tp_y(dy))

    def last_x(step, *dys):
        if step == 3:
            take(("lx2",), column_of(pl.ds(0, 8), xm(2), pl.ds(*LAST)))
        for dy in dys:
            yy, cut = ym(-dy), 1 + DYS.index(dy) % 2
            if step == 1 and dy:
                take(("ly", dy), x_buf.at[yy, pair, half, pl.ds(*LAST)])
            for w in WAYS:
                ps = pl.ds(*LAST)
                piece = pl.ds(*part((*LAST, cut), w))
                xx = xm(-w * (step - 1))
                if step == 2:
                    take(("lx1", dy, w), column_of(yy, xx, ps))
                    ps = piece
                src = column_of(yy, xx, ps)
                send(("lx1", dy, w) if step == 1 else ("lx2",), src, src, ep, tp_x(w))

    def up(yy, first, start):
        weights = wgu[pl.ds(pl.multiple_of(yy * 256, 256), 256), :]
        ps = pl.ds(first, 6)
        left = jnp.concatenate(
            [
                jnp.concatenate(
                    [x_buf[yy, t, h, ps].reshape(96, 128) for t in range(2)], axis=1
                )
                for h in range(2)
            ],
            axis=0,
        )
        term = jnp.dot(left, weights, preferred_element_type=F32)
        acc[...] = term if start else acc[...] + term

    def act():
        gate, upv = acc[:, :384], acc[:, 384:]
        return (gate / (1.0 + jnp.exp(-gate)) * upv).astype(BF)

    def down(hidden, dy, first):
        yy = ym(dy)
        cols = pl.ds(pl.multiple_of(yy * 256, 256), 256)
        term = jnp.dot(hidden, wdn[:, cols], preferred_element_type=F32).astype(BF)
        for xx in range(NX):
            h, t = xx % 2, xx // 2
            block = term[96 * h : 96 * (h + 1), 128 * t : 128 * (t + 1)]
            y_buf[yy, xx, pl.ds(first, 6)] = block.reshape(6, 16, 128)

    def own(yy, xx, span):
        return y_buf[yy, xx, pl.ds(span[0], span[1])].astype(F32)

    def local(span, w):
        s = part(span, w)
        return pl.ds(s[0] - span[0], s[1])

    def whole(span):
        return pl.ds(0, span[1])

    def other(span, w):
        return local(span, -w)

    def ray(step):
        for dx in DXS:
            i = DXS.index(dx)
            for w in WAYS:
                d = 0 if w > 0 else 1
                yy = ym(w * (5 - step))
                if step == 1:
                    src = y_buf.at[yy, xm(dx), pl.ds(*part(RA, w))]
                    send(("ray", 1, dx, w), src, ra_y.at[d, 0, i, local(RA, w)], ep, tp_y(w))
                    continue
                if step == 2:
                    got = ra_y.at[d, 0, i, local(RA, w)]
                    take(("ray", 1, dx, w), got)
                    sa_y[d, 0, i, local(RA, w)] = (own(yy, xm(dx), part(RA, w)) + got[...].astype(F32)).astype(BF)
                    sa_y[d, 0, i, other(RA, w)] = y_buf[yy, xm(dx), pl.ds(*part(RA, -w))]
                else:
                    got = ra_y.at[d, step - 2, i]
                    take(("ray", step - 1, dx, w), got)
                    sa_y[d, step - 2, i] = (own(yy, xm(dx), RA) + got[...].astype(F32)).astype(BF)
                key = ("ray", 4, dx) if step == 4 else ("ray", step, dx, w)
                send(key, sa_y.at[d, step - 2, i], ra_y.at[d, step - 1, i], ep, tp_y(w))

    def ray_end(dx):
        i = DXS.index(dx)
        take(("ray", 4, dx), ra_y.at[:, 3, i])
        total = own(y, xm(dx), RA) + ra_y[0, 3, i].astype(F32) + ra_y[1, 3, i].astype(F32)
        za[i] = total.astype(BF)

    def rax(dx):
        i = DXS.index(dx)
        send(("rax",), za.at[i], ra_x.at[i], ep, tp_x(dx))

    def rax_end():
        total = za[3].astype(F32)
        take(("rax",), ra_x)
        for i in range(3):
            total = total + ra_x[i].astype(F32)
        res[pl.ds(RA[0], RA[1])] = total.astype(BF)

    def rbx(step, dy):
        i, yy = DYS.index(dy), ym(dy)
        for w in WAYS:
            d = 0 if w > 0 else 1
            here = local(RB, w)
            if step == 1:
                src = y_buf.at[yy, xm(2), pl.ds(*part(RB, w))]
                send(("rbx", 1, dy, w), src, rb_x.at[i, d, 0, here], ep, tp_x(w))
            elif step == 2:
                got = rb_x.at[i, d, 0, here]
                take(("rbx", 1, dy, w), got)
                sb_x[i, d, here] = (own(yy, xm(w), part(RB, w)) + got[...].astype(F32)).astype(BF)
                sb_x[i, d, other(RB, w)] = y_buf[yy, xm(w), pl.ds(*part(RB, -w))]
                send(("rbx", 2, dy), sb_x.at[i, d], rb_x.at[i, d, 1], ep, tp_x(w))
        if step == 3:
            take(("rbx", 2, dy), rb_x.at[i, :, 1])
            total = own(yy, x, RB) + rb_x[i, 0, 1].astype(F32) + rb_x[i, 1, 1].astype(F32)
            zb[i] = total.astype(BF)

            if i < 7:
                send(("rby",), zb.at[i], rb_y.at[i], ep, tp_y(dy))

    def rby_end():
        total = zb[7].astype(F32)
        take(("rby",), rb_y)
        for i in range(7):
            total = total + rb_y[i].astype(F32)
        res[pl.ds(RB[0], RB[1])] = total.astype(BF)

    gather_y(0, 1)
    gather_y(1, 1)
    hand_on(*LEGS)
    gather_y(2, 1)
    gather_y(0, 2)
    gather_y(1, 2)
    last_y(DYS[1:7])
    last_x(1, 0)
    gather_y(2, 2)
    gather_x(1)
    gather_y(0, 3)
    last_y(DYS[:1])
    gather_y(1, 3)
    last_x(1, 1, -1)
    gather_y(2, 3)
    gather_x(2)
    gather_y(0, 4)
    last_x(1, 2, -2)
    gather_y(1, 4)
    gather_y(2, 4)
    last_x(1, 3, -3, 4)
    take(("near",), x_buf.at[:, :, 1 - core, 0])
    loads[4].wait()
    loads[5].wait()
    for dy in (0, 1, -1):
        up(ym(dy), 0, dy == 0)
    last_x(2, 0, 1, -1)
    for dy in (2, -2):
        up(ym(dy), 0, False)
    last_x(2, 2, -2)
    for dy in (3, -3):
        up(ym(dy), 0, False)
    for chunk in range(3):
        gather_y(chunk, 5)
    up(ym(4), 0, False)
    hidden = act()
    loads[6].wait()
    down(hidden, 4, 0)
    ray(1)
    for dy in DYS[1:4]:
        down(hidden, dy, 0)
    last_x(2, 3, -3, 4)
    for dy in DYS[4:]:
        down(hidden, dy, 0)
    gather_x(3)
    ray(2)
    last_x(3)
    for yy in range(NY):
        up(yy, 6, yy == 0)
    hidden = act()
    for dy in DYS[:4]:
        down(hidden, dy, 6)
        rbx(1, dy)
    ray(3)
    for dy in DYS[4:]:
        down(hidden, dy, 6)
        rbx(1, dy)
    for dy in DYS:
        rbx(2, dy)
    ray(4)
    for dy in DYS[:3]:
        rbx(3, dy)
    for dx, dys in zip(DXS, ((2, -2), (1, -1), (0,), ())):
        for dy in dys:
            rbx(3, dy)
        ray_end(dx)
        if dx:
            rax(dx)

    def give(span):
        for p in range(span[0] + span[1] - 1, span[0] - 1, -1):
            e = 2 * zm(OFF[p]) + half
            send(("back",), res.at[p], back.at[p, core], e, twin)
            if p > 0:
                send(("back",), res.at[p], back.at[p, core], e, tp)

    rby_end()
    give(RB)
    rax_end()
    give(RA)
    near_back = message(("back",), res.at[0], back.at[0, core], 2 * z + half, tp, 2)

    @pl.when(half == core)
    def _():
        back[0, core] = res[0]
        take(("back",), pool.at[pl.ds(0, 23)])

    @pl.when(half != core)
    def _():
        near_back.start()
        take(("back",), pool.at[pl.ds(0, 24)])
        wait_sent(2, 1)

    rows_in = back[...].reshape(384, 128)
    mixed = jnp.dot(comb_hi[...], rows_in, preferred_element_type=F32)
    mixed = mixed + jnp.dot(comb_lo[...], rows_in, preferred_element_type=F32)
    mixed = jnp.transpose(mixed)
    out[...] = jnp.where(half == 1, mixed[64:], mixed[:64]).astype(BF)

    wait_sent(0, sum(sent))

    @pl.when(core == half)
    def _():
        wait_sent(1, sum(n for _, n in sent_z))

    assert len(places) == N_TAKE and sum(sent) <= POOL, (len(places), sum(sent))


def per_device(tokens, norm_gain, route_ids, route_weights, gate_proj, up_proj, down_proj):
    vmem = pl.BlockSpec(memory_space=pltpu.VMEM)
    hbm = pl.BlockSpec(memory_space=pl.ANY)

    def tiles(*lead):
        return pltpu.VMEM((*lead, 16, 128), BF)

    a, b = RA[1], RB[1]
    return pl.pallas_call(
        kernel,
        out_shape=jax.ShapeDtypeStruct((64, 128), BF),
        in_specs=[hbm] * 7,
        out_specs=vmem,
        scratch_shapes=[
            pltpu.VMEM((128, 2048), BF),
            pltpu.VMEM((1, 2048), F32),
            pltpu.VMEM((2, 128), jnp.int32),
            pltpu.VMEM((2, 128), F32),
            tiles(NY, 2, 2, NZ),
            pltpu.VMEM((128, 2048), BF),
            tiles(5, 2, 2),
            tiles(6, 2, NY),
            tiles(2, NY),
            tiles(3),
            tiles(NY, 2),
            pltpu.VMEM((2048, 768), BF),
            pltpu.VMEM((384, 2048), BF),
            pltpu.VMEM((192, 768), F32),
            tiles(NY, NX, NZ),
            pltpu.VMEM((128, 384), BF),
            pltpu.VMEM((128, 384), BF),
            tiles(2, 4, 4, a), tiles(2, 3, 4, a), tiles(4, a), tiles(3, a),
            tiles(8, 2, 2, b), tiles(8, 2, b), tiles(8, b), tiles(7, b),
            tiles(NZ),
            tiles(NZ, 2),
            tiles(POOL),
            pltpu.SemaphoreType.DMA((7,)),
            pltpu.SemaphoreType.DMA((3,)),
            pltpu.SemaphoreType.DMA((N_TAKE,)),
        ],
        compiler_params=pltpu.CompilerParams(collective_id=0, has_side_effects=True),
        cost_estimate=pl.CostEstimate(
            flops=2_000_000_000, bytes_accessed=6_000_000, transcendentals=200_000
        ),
    )(
        tokens, norm_gain.reshape(1, -1), route_ids.T, route_weights.T,
        gate_proj, up_proj, down_proj,
    ).T


def solution(mesh):
    placed = (
        P("ep", None),
        P(),
        P("ep", None),
        P("ep", None),
        P("ep", None, "tp"),
        P("ep", None, "tp"),
        P("ep", "tp", None),
    )
    return jax.shard_map(
        per_device, mesh=mesh, in_specs=placed, out_specs=P("ep", "tp"), check_vma=False
    )
```
